256 devices in a mesh: grp: 4 (over y, x), ep: 32 (over z), tp: 2 (over core).
Axes of the slice: x: 2, y: 2, z: 32, core: 2. Of those that a mesh axis runs over, the one named last changes fastest.
The devices are a block of a 4x16x32 slice.
Arguments:
- tokens: bfloat16 [32768, 2048], P(('grp', 'ep', 'tp')), parts along dimension 0, may hold values from -6 to 6
- expert_ids: int32 [32768, 4], P(('grp', 'ep', 'tp')), parts along dimension 0, may hold values from 0 to 63, all different within a row; in each aligned block of 128 rows (0 to 127, 128 to 255, ...) at most 16 rows name the same one
- route_weights: float32 [32768, 4], P(('grp', 'ep', 'tp')), parts along dimension 0, may hold values from 0.05 to 1
- norm_gain: float32 [2048], replicated, may hold values from 0.1 to 1.9
- w_gate: bfloat16 [64, 2048, 896], P(('ep', 'tp')), may hold values from -0.5 to 0.5
- w_up: bfloat16 [64, 2048, 896], P(('ep', 'tp')), may hold values from -0.5 to 0.5
- w_down: bfloat16 [64, 896, 2048], P(('ep', 'tp')), may hold values from -0.0234375 to 0.0234375
Outputs:
- mixed: bfloat16 [32768, 2048], P(('grp', 'ep', 'tp')), parts along dimension 0
The draws below stay inside these ranges and needn't reach their ends.
There are 4 independent parts, one for each index of `grp`. The reference program is written for one: setup_inputs(seed, part) draws one part's arguments, and reference() takes and returns one part's arrays. A program takes and returns all parts, laid end to end along the dimension named above; an argument that names none is the same for every part. Nothing has to cross between parts.
Inputs may be any that keep to these rules, and one draw needn't show every extreme that they name: `expert_ids`: each token names 4 different experts. Among the 128 tokens of one device (aligned blocks of rows) no expert is named more than 16 times, a bound that some block reaches.
All inputs are finite; a program needn't handle non-finite values.
Results may differ from the reference program's by a relative error of at most 0.0071.
Values may be sent and summed in bfloat16 or wider, within the bound.
A program may use at most 64 MiB of HBM per device.

```python
import math
import jax
import jax.numpy as jnp
import numpy as np
from jax import lax

D = 2048
F = 896
TOPK = 4
TOK_DEV = 128
EXPERTS = 64
CAP = 16
TOKENS = 8192
N_EP = 32
N_TP = 2


def level_of(key, dims, cuts, smallest, high):
    factor_of = 1.0
    for dim, blocks in cuts:
        draws = jax.random.uniform(jax.random.fold_in(jax.random.fold_in(key, 6), dim), (blocks,), jnp.float32, smallest / len(cuts), high / len(cuts))
        factor_of = factor_of * jnp.repeat(jnp.exp(draws), dims[dim] // blocks).reshape((-1,) + (1,) * (len(dims) - 1 - dim))
    return factor_of


def shared_out(own_key, own, number, rows, amount, top, bound, slope):
    ranking = jax.random.permutation(own_key, amount)
    crowded, common = load_shares(amount, rows * top, bound, slope, True), load_shares(amount, rows * top, bound, slope, False)
    places = jnp.arange(amount)

    def named(sizes, turn):
        used = int((sizes > 0).sum())
        fixed = max(1, used // 4)
        shifted = fixed + (places - fixed + turn * (used - fixed)) % max(1, amount - fixed)
        return jnp.zeros((amount,), jnp.int32).at[ranking[jnp.where(places < fixed, places, shifted)]].set(jnp.asarray(sizes, jnp.int32))

    sizes = jnp.where(number % 4 == 0, named(crowded, number // 4), named(common, number - number // 4 - 1))
    mixed = jax.random.permutation(jax.random.fold_in(own, 3), amount)
    source_of, receiver = mixed[0:amount // 2 * 2:2], mixed[1:amount // 2 * 2:2]
    room = jnp.minimum(sizes[source_of] - 1, bound - sizes[receiver]) // 2
    room = jnp.where((source_of == ranking[0]) | (receiver == ranking[0]) | (sizes[receiver] == 0), 0, jnp.maximum(room, 0))
    shifted = jax.random.randint(jax.random.fold_in(own, 4), (amount // 2,), 0, 1 << 20) % (room + 1)
    sizes = sizes.at[source_of].add(-shifted).at[receiver].add(shifted)
    items = jnp.searchsorted(jnp.cumsum(sizes), jnp.arange(rows * top), side="right").astype(jnp.int32)
    grid = items.reshape(top, rows).T
    grid = grid[jax.random.permutation(jax.random.fold_in(own, 1), rows)]
    turn = jax.random.randint(jax.random.fold_in(own, 2), (rows, 1), 0, top)
    return jnp.take_along_axis(grid, (jnp.arange(top)[None, :] + turn) % top, axis=1)


def load_shares(amount, total, limit, lean, full):
    loads = [(1 << 20) // math.isqrt(standing ** lean) + 1 for standing in range(1, amount + 1)]
    largest = limit if full else min(limit, max(-(-total // amount), total * loads[0] // sum(loads)))
    least = 1 if total - largest >= amount - 1 else 0
    given, surplus = [largest] + [least] * (amount - 1), total - largest - least * (amount - 1)
    while surplus > 0:
        free = [i for i in range(1, amount) if given[i] < largest] or [i for i in range(1, amount) if given[i] < limit]
        whole, left = sum([loads[i] for i in free]), surplus
        for i in free:
            extra = min(limit - given[i], max(1, left * loads[i] // whole), surplus)
            given[i] = given[i] + extra
            surplus = surplus - extra
    return np.array(given)


def noise(stream_key, shape, scale, limit, cuts=(), kind=jnp.bfloat16):
    gain = level_of(stream_key, shape, cuts, -0.22, 0.18) if cuts else 1.0
    values = jax.random.normal(stream_key, shape, jnp.float32) * scale * gain
    return jnp.minimum(jnp.maximum(values, -limit), limit).astype(kind)


def setup_inputs(seed: int = 0, part: int = 0) -> dict:
    splits = jax.random.split(jax.random.key(seed), 8)
    part_splits = jax.random.split(jax.random.fold_in(splits[7], part), 8)
    tokens = noise(part_splits[0], (TOKENS, D), 1.0, 6.0, ((0, 64),))
    expert_ids_keys = jax.random.split(jax.random.fold_in(part_splits[1], 1), TOKENS // TOK_DEV)
    expert_ids_turns = jax.random.permutation(jax.random.fold_in(part_splits[1], 3), TOKENS // TOK_DEV)
    expert_ids = jax.vmap(lambda own, number: shared_out(jax.random.fold_in(part_splits[1], 2), own, number, TOK_DEV, EXPERTS, TOPK, CAP, 2))(expert_ids_keys, expert_ids_turns).reshape((TOKENS, TOPK))
    route_weights = jnp.clip(jnp.exp(math.log(1.0) - 2.9957323 * jax.random.uniform(part_splits[2], (TOKENS, TOPK), jnp.float32) ** level_of(part_splits[2], (TOKENS, TOPK), ((0, 64),), -0.2, 0.2)), 0.05, 1.0)
    norm_gain = jnp.clip(1.0 + 0.18 * jax.random.normal(splits[3], (D,), jnp.float32), 0.1, 1.9)
    w_gate = noise(splits[4], (EXPERTS, D, F), (D // 16) ** -0.5, 0.5, ((0, 64),))
    w_up = noise(splits[5], (EXPERTS, D, F), (D // 16) ** -0.5, 0.5, ((0, 64),))
    w_down = noise(splits[6], (EXPERTS, F, D), (64 * F) ** -0.5, 0.0234375, ((0, 64),))
    return {"tokens": tokens, "expert_ids": expert_ids, "route_weights": route_weights, "norm_gain": norm_gain, "w_gate": w_gate, "w_up": w_up, "w_down": w_down}


norm_eps = 1e-05
clamp_limit = 7.0
sig_alpha = 1.702

def layer_norm(tokens, norm_gain):
    values = tokens.astype(jnp.float32)
    row_mean = lax.optimization_barrier(jnp.mean(values, -1, keepdims=True))
    centred = values - row_mean
    row_var = lax.optimization_barrier(jnp.mean(centred * centred, -1, keepdims=True))
    scaled = centred * lax.rsqrt(row_var + norm_eps) * norm_gain.astype(jnp.float32)
    return scaled.astype(jnp.bfloat16)

def expert_apply(inputs, gate_mat, up_mat, down_mat):
    gate_pre = jnp.dot(inputs, gate_mat, preferred_element_type=jnp.float32)
    up_pre = jnp.dot(inputs, up_mat, preferred_element_type=jnp.float32)
    gated = jnp.minimum(gate_pre, clamp_limit)
    upper = jnp.clip(up_pre, -clamp_limit, clamp_limit)
    hidden = (gated * jax.nn.sigmoid(sig_alpha * gated) * (upper + 1.0)).astype(jnp.bfloat16)
    return jnp.dot(hidden, down_mat, preferred_element_type=jnp.float32).astype(jnp.bfloat16)

def reference(tokens, expert_ids, route_weights, norm_gain, w_gate, w_up, w_down):
    normed = layer_norm(tokens, norm_gain)
    flat_ids = expert_ids.reshape(-1).astype(jnp.int32)
    sorted_pairs = jnp.argsort(flat_ids, stable=True).astype(jnp.int32)
    counts = lax.optimization_barrier(jnp.sum((flat_ids[:, None] == jnp.arange(EXPERTS, dtype=jnp.int32)[None, :]).astype(jnp.int32), 0))
    starts = (jnp.cumsum(counts) - counts).astype(jnp.int32)
    slot_limit = N_EP * N_TP * CAP
    padded = jnp.concatenate([sorted_pairs, jnp.zeros((slot_limit,), jnp.int32)])
    pair_weights = route_weights.reshape(-1).astype(jnp.float32)

    def add_expert(accum_total, inputs):
        expert, gate_mat, up_mat, down_mat = inputs
        pair_index = lax.dynamic_slice_in_dim(padded, starts[expert].astype(jnp.int32), slot_limit)
        live_mask = jnp.arange(slot_limit, dtype=jnp.int32) < counts[expert]
        token_index = (pair_index // TOPK).astype(jnp.int32)
        results = expert_apply(normed[token_index], gate_mat, up_mat, down_mat)
        factor = jnp.where(live_mask, pair_weights[pair_index], jnp.zeros((), jnp.float32))
        scaled = factor[:, None] * results.astype(jnp.float32)
        return (accum_total.at[token_index].add(scaled), None)
    start_total = jnp.zeros((TOKENS, D), jnp.float32)
    accum_total, unused = lax.scan(add_expert, start_total, (jnp.arange(EXPERTS, dtype=jnp.int32), w_gate, w_up, w_down))
    return accum_total.astype(jnp.bfloat16)
```

```python
import functools

import jax
import jax.numpy as jnp
from jax import lax
from jax.experimental import pallas as pl
from jax.experimental.pallas import tpu as pltpu
from jax.sharding import PartitionSpec as P

norm_eps = 1e-05
clamp_limit = 7.0
sig_alpha = 1.702

F32 = jnp.float32
BF16 = jnp.bfloat16
VMEM_BYTES = 67_043_328


def iota(shape, dim):
    return lax.broadcasted_iota(jnp.int32, shape, dim)


def dot(a, b):
    return jnp.dot(a, b, preferred_element_type=F32)


def routed_kernel(
    cap,
    tokens_ref, ids_ref, gates_ref, gain_ref, wg_hbm, wu_hbm, wd_hbm,
    out_ref,
    wgu, wd, xn, unsort,
    ag0, ag1, rs0, rs1, md0, md1, st0, st1,
    xin, xout, yy, yout,
    w_sem, ag_rv0, ag_rv1, rs_rv0, rs_rv1, md_rv0, md_rv1, x_rv, y_rv,
    ag_tx, rs_tx, md_tx, x_tx, y_tx,
):
    n = lax.axis_size("ep")
    cores = lax.axis_size("tp")
    me = lax.axis_index("ep")
    core = lax.axis_index("tp")
    rows, width = tokens_ref.shape
    top = ids_ref.shape[0]
    hidden_width = wg_hbm.shape[2]
    experts = n * cores
    quad = cores * cap
    parts = rows // quad
    reach = (n // 2, n - 1 - n // 2)
    batch = 2 * quad
    ag, rs, md, st = (ag0, ag1), (rs0, rs1), (md0, md1), (st0, st1)
    ag_rv, rs_rv, md_rv = (ag_rv0, ag_rv1), (rs_rv0, rs_rv1), (md_rv0, md_rv1)

    turn = 1 - 2 * core
    nxt = (lax.rem(me + turn + n, n), lax.rem(me - turn + n, n))
    partner = {"tp": 1 - core}

    def copy_to(src, dst, tx, rv, device):
        return pltpu.make_async_remote_copy(
            src_ref=src, dst_ref=dst, send_sem=tx, recv_sem=rv,
            device_id=device, device_id_type=pl.DeviceIdType.MESH,
        )

    loads = (
        pltpu.make_async_copy(wg_hbm.at[0], wgu.at[:, pl.ds(0, hidden_width)], w_sem.at[0]),
        pltpu.make_async_copy(wu_hbm.at[0], wgu.at[:, pl.ds(hidden_width, hidden_width)], w_sem.at[1]),
        pltpu.make_async_copy(wd_hbm.at[0], wd, w_sem.at[2]),
    )
    for load in loads:
        load.start()

    barrier = pltpu.get_barrier_semaphore()
    for device in ({"ep": nxt[0]}, {"ep": nxt[1]}, partner):
        pl.semaphore_signal(barrier, inc=1, device_id=device, device_id_type=pl.DeviceIdType.MESH)

    def norm_rows(g, carry):
        at = pl.ds(pl.multiple_of(g * 16, 16), 16)
        values = tokens_ref[at, :].astype(F32)
        centred = values - jnp.mean(values, -1, keepdims=True)
        var = jnp.mean(centred * centred, -1, keepdims=True)
        xn[at, :] = (centred * lax.rsqrt(var + norm_eps) * gain_ref[...]).astype(BF16)
        return carry

    lax.fori_loop(0, rows // 16, norm_rows, 0)

    ids = ids_ref[...]
    lane = iota((1, rows), 1)
    hits = [ids[k:k + 1] == iota((experts, rows), 0) for k in range(top)]
    named = functools.reduce(jnp.add, [h.astype(F32) for h in hits])
    earlier = (iota((rows, rows), 0) < iota((rows, rows), 1)).astype(BF16)
    before = dot(named.astype(BF16), earlier)
    slots = [jnp.sum(jnp.where(h, before, 0.0), 0, keepdims=True) for h in hits]
    codes = [(cap * ids[k:k + 1]).astype(F32) + slots[k] for k in range(top)]
    meta = jnp.concatenate(codes + [gates_ref[k:k + 1] for k in range(top)], 0)
    meta_hi = meta.astype(BF16)
    rest = meta - meta_hi.astype(F32)
    meta_mid = rest.astype(BF16)
    meta_lo = (rest - meta_mid.astype(F32)).astype(BF16)

    away = lax.rem((ids // cores - me) * turn + 2 * n, n)
    eye = iota((rows, rows), 0) == iota((rows, rows), 1)
    place = []
    for d in range(2):
        far = away if d == 0 else n - away
        inside = (away <= reach[0]) if d == 0 else (away > reach[0])
        far = jnp.max(jnp.where(inside, far, 0), 0, keepdims=True)
        key = (far * rows + (rows - 1 - lane)).astype(F32)
        key_col = jnp.sum(jnp.where(eye, key, 0.0), 1, keepdims=True)
        rank = jnp.sum((key_col > key).astype(F32), 0, keepdims=True)
        rank_col = jnp.sum((key > key_col).astype(F32), 1, keepdims=True)
        place.append((iota((rows, rows), 0).astype(F32) == rank).astype(BF16))
        back = (iota((rows, rows), 1).astype(F32) == rank_col).astype(BF16)
        unsort[d] = back
        md[d][0:8, :] = dot(meta_hi, back) + dot(meta_mid, back) + dot(meta_lo, back)

    def sort_part(i):
        for d in range(2):
            ag[d][quad * i:quad * (i + 1), :] = dot(
                place[d][quad * i:quad * (i + 1)], xn[...]
            ).astype(BF16)

    for d in range(2):
        for short in range(1, parts):
            h = reach[d] - parts + 1 + short
            top_row = rows * h + quad * (parts - short)
            ag[d][top_row:rows * (h + 1), :] = jnp.zeros((quad * short, width), BF16)
    for j in (0, reach[0]):
        xin[batch * j + cap:batch * j + 2 * cap, :] = jnp.zeros((cap, width), BF16)
        xout[quad * j + cap:quad * (j + 1), :] = jnp.zeros((cap, width), BF16)

    def send_part(d, i, h):
        at = pl.multiple_of(rows * (h - 1) + quad * i, quad)
        if i == 0:
            m = pl.multiple_of(8 * (h - 1), 8)
            copy_to(md[d].at[pl.ds(m, 8)], md[d].at[pl.ds(m + 8, 8)],
                    md_tx.at[d], md_rv[d].at[h], {"ep": nxt[d]}).start()
        copy_to(ag[d].at[pl.ds(at, quad)], ag[d].at[pl.ds(at + rows, quad)],
                ag_tx.at[d], ag_rv[d].at[h, i], {"ep": nxt[d]}).start()

    def take_part(d, i, h):
        at = pl.multiple_of(rows * h + quad * i, quad)
        if i == 0:
            m = md[d].at[pl.ds(pl.multiple_of(8 * h, 8), 8)]
            copy_to(m, m, md_tx.at[d], md_rv[d].at[h], {"ep": nxt[d]}).wait_recv()
        part = ag[d].at[pl.ds(at, quad)]
        copy_to(part, part, ag_tx.at[d], ag_rv[d].at[h, i], {"ep": nxt[d]}).wait_recv()

    def select_rows(d, j, meta, block):
        row = iota((quad, rows), 0)
        want = (quad * me + lax.rem(cap * core + row, quad)).astype(F32)
        pick = jnp.zeros((quad, rows), F32)
        weight = jnp.zeros((quad, rows), F32)
        for k in range(top):
            hit = meta[k:k + 1] == want
            pick = jnp.where(hit, 1.0, pick)
            weight = jnp.where(hit, meta[top + k:top + k + 1], weight)
        found = dot(pick.astype(BF16), block).astype(BF16)
        xin[pl.ds(pl.multiple_of(batch * j + cap * d, cap), cap), :] = found[:cap]
        xout[pl.ds(pl.multiple_of(quad * j + cap * d, cap), cap), :] = found[cap:]
        none = jnp.zeros((cap, rows), F32)
        mine, other = weight[:cap], weight[cap:]
        spread = (mine, none, other, none) if d == 0 else (none, mine, none, other)
        spread = jnp.concatenate(spread + (jnp.zeros((rows - batch, rows), F32),), 0)
        st[d][pl.ds(pl.multiple_of(rows * j, rows), rows), :] = spread.T.astype(BF16)

    def select_block(d, j):
        at = pl.multiple_of(rows * j, rows)
        select_rows(d, j, md[d][pl.ds(pl.multiple_of(8 * j, 8), 8), :], ag[d][pl.ds(at, rows), :])

    def x_copy(j):
        return copy_to(xout.at[pl.ds(pl.multiple_of(quad * j, quad), quad)],
                       xin.at[pl.ds(pl.multiple_of(batch * j + quad, quad), quad)],
                       x_tx, x_rv.at[j], partner)

    def y_copy(j):
        return copy_to(yout.at[pl.ds(pl.multiple_of(quad * j, quad), quad)],
                       yy.at[pl.ds(pl.multiple_of(batch * j + quad, quad), quad)],
                       y_tx, y_rv.at[j], partner)

    def expert_batch(j):
        x_copy(j).wait_recv()
        at = pl.multiple_of(batch * j, batch)
        pre = dot(xin[pl.ds(at, batch), :], wgu[...])
        gated = jnp.minimum(pre[:, :hidden_width], clamp_limit)
        upper = jnp.clip(pre[:, hidden_width:], -clamp_limit, clamp_limit)
        hidden = (gated * jax.nn.sigmoid(sig_alpha * gated) * (upper + 1.0)).astype(BF16)
        result = dot(hidden, wd[...]).astype(BF16)
        yy[pl.ds(at, quad), :] = result[:quad]
        yout[pl.ds(pl.multiple_of(quad * j, quad), quad), :] = result[quad:]
        y_copy(j).start()

    sort_part(0)
    pl.semaphore_wait(barrier, 3)
    both = (0, 1)
    for d in both:
        send_part(d, 0, 1)
    sort_part(1)
    for d in both:
        send_part(d, 1, 1)
    sort_part(2)
    sort_part(3)
    for d in both:
        take_part(d, 0, 1)
        send_part(d, 0, 2)
    select_rows(0, 0, meta, xn[...])
    x_copy(0).start()
    for d in both:
        take_part(d, 1, 1)
        send_part(d, 1, 2)
    for d in both:
        take_part(d, 0, 2)
        send_part(d, 0, 3)
    for d in both:
        send_part(d, 2, 1)
    for i in range(3):
        for d in both:
            take_part(d, i, 3 - i)
            send_part(d, i, 4 - i)
    for d in both:
        send_part(d, 3, 1)
    for load in loads:
        load.wait()

    def round_of(r, moving):
        for i in range(parts):
            h = r + 2 - i
            for d in both:
                take_part(d, i, h)
                if d in moving:
                    send_part(d, i, h + 1)
            if i == 0:
                expert_batch(r - 2)
        for d in both:
            select_block(d, r - 1)
        x_copy(r - 1).start()

    def round_body(r, carry):
        round_of(r, both)
        return carry

    last = reach[1] - parts + 1
    lax.fori_loop(2, last + 1, round_body, 0)
    round_of(last + 1, (0,))
    for j in range(last + 1, reach[1] + 1):
        select_block(1, j)
    expert_batch(last)
    for i in range(parts):
        take_part(0, i, reach[0] - i)
        select_block(0, reach[0] - i)
        x_copy(reach[0] - i).start()

    def y_wait(j):
        y_copy(j).wait_recv()

    def give_part(d, j, i, fresh=False):
        at = pl.multiple_of(rows * j + quad * i, quad)
        share = dot(st[d][pl.ds(at, quad), :][:, :batch], yy[pl.ds(pl.multiple_of(batch * j, batch), batch), :])
        part = rs[d].at[pl.ds(at, quad)]
        if not fresh:
            copy_to(part, part, rs_tx.at[d], rs_rv[d].at[j, i], {"ep": nxt[d]}).wait_recv()
            share = share + part[...].astype(F32)
        part[...] = share.astype(BF16)
        copy_to(part, rs[d].at[pl.ds(at - rows, quad)], rs_tx.at[d], rs_rv[d].at[j - 1, i],
                {"ep": nxt[1 - d]}).start()

    def y_wait_body(j, carry):
        y_wait(j)
        return carry

    lax.fori_loop(0, last + 1, y_wait_body, 0)
    give_part(1, last, parts - 1, True)

    def turn_body(t, carry):
        expert_batch(reach[0] - t)

        @pl.when(t >= 1)
        def _():
            y_wait(reach[0] + 1 - t)
            give_part(0, reach[0] + 1 - t, t - 1, True)

        @pl.when(t >= 2)
        def _():
            give_part(1, reach[0] + 1 - t, t - 2, True)

        return carry

    lax.fori_loop(0, parts, turn_body, 0)
    y_wait(last + 1)
    give_part(0, last + 1, parts - 1, True)
    give_part(1, last + 1, parts - 2, True)

    def give_body(r, carry):
        for i in range(parts):
            for d in both:
                give_part(d, reach[d] - i - r, i)
        return carry

    lax.fori_loop(1, last, give_body, 0)
    closing = ((3, 0), (2, 1), (1, 2), (2, 0), (1, 1), (1, 0))
    order0 = tuple((parts - i, i) for i in range(parts)) + closing
    for step in range(len(order0)):
        give_part(0, *order0[step])
        if step < len(closing):
            give_part(1, *closing[step])

    for d in both:
        for i in range(parts):
            part = rs[d].at[pl.ds(quad * i, quad)]
            copy_to(part, part, rs_tx.at[d], rs_rv[d].at[0, i], {"ep": nxt[d]}).wait_recv()
    mixed = dot(st0[0:rows, :][:, :batch], yy[0:batch, :])
    for d in both:
        mixed = mixed + dot(unsort[d], rs[d][0:rows, :])
    out_ref[...] = mixed.astype(BF16)

    for d in both:
        moved = quad * sum(reach[d] - i for i in range(parts))
        sent = ag[d].at[pl.ds(0, moved)]
        copy_to(sent, sent, ag_tx.at[d], ag_rv[d].at[0, 0], {"ep": nxt[d]}).wait_send()
        sent = rs[d].at[pl.ds(0, moved)]
        copy_to(sent, sent, rs_tx.at[d], rs_rv[d].at[0, 0], {"ep": nxt[d]}).wait_send()
        sent = md[d].at[pl.ds(0, 8 * reach[d])]
        copy_to(sent, sent, md_tx.at[d], md_rv[d].at[0], {"ep": nxt[d]}).wait_send()
    copy_to(xout, xout, x_tx, x_rv.at[0], partner).wait_send()
    copy_to(yout, yout, y_tx, y_rv.at[0], partner).wait_send()


def local(tokens, expert_ids, route_weights, norm_gain, w_gate, w_up, w_down):
    n = lax.axis_size("ep")
    cores = lax.axis_size("tp")
    rows, width = tokens.shape
    top = expert_ids.shape[1]
    hidden_width = w_gate.shape[2]
    cap = 2 * rows * top // (n * cores)
    quad = cores * cap
    parts = rows // quad
    reach = (n // 2, n - 1 - n // 2)
    batches = reach[0] + 1
    vmem = pl.BlockSpec(memory_space=pltpu.VMEM)
    hbm = pl.BlockSpec(memory_space=pl.ANY)
    dma = pltpu.SemaphoreType.DMA
    blocks = [pltpu.VMEM((rows * (r + 1), width), BF16) for r in reach]
    return pl.pallas_call(
        functools.partial(routed_kernel, cap),
        name="routed_layer",
        out_shape=jax.ShapeDtypeStruct((rows, width), BF16),
        in_specs=[vmem] * 4 + [hbm] * 3,
        out_specs=vmem,
        scratch_shapes=[
            pltpu.VMEM((width, 2 * hidden_width), BF16),
            pltpu.VMEM((hidden_width, width), BF16),
            pltpu.VMEM((rows, width), BF16),
            pltpu.VMEM((2, rows, rows), BF16),
            *blocks,
            *blocks,
            *[pltpu.VMEM((8 * (r + 1), rows), F32) for r in reach],
            *[pltpu.VMEM((rows * (r + 1), rows), BF16) for r in reach],
            pltpu.VMEM((2 * quad * batches, width), BF16),
            pltpu.VMEM((quad * batches, width), BF16),
            pltpu.VMEM((2 * quad * batches, width), BF16),
            pltpu.VMEM((quad * batches, width), BF16),
            dma((3,)),
            *[dma((r + 1, parts)) for r in reach],
            *[dma((r + 1, parts)) for r in reach],
            *[dma((r + 1,)) for r in reach],
            dma((batches,)),
            dma((batches,)),
            dma((2,)),
            dma((2,)),
            dma((2,)),
            dma,
            dma,
        ],
        compiler_params=pltpu.CompilerParams(
            collective_id=0, has_side_effects=True, vmem_limit_bytes=VMEM_BYTES
        ),
    )(tokens, expert_ids.T, route_weights.T, norm_gain.reshape(1, width), w_gate, w_up, w_down)


def solution(mesh):
    placed = (
        P(("grp", "ep", "tp"), None),
        P(("grp", "ep", "tp"), None),
        P(("grp", "ep", "tp"), None),
        P(),
        P(("ep", "tp"), None, None),
        P(("ep", "tp"), None, None),
        P(("ep", "tp"), None, None),
    )
    return jax.shard_map(
        local, mesh=mesh, in_specs=placed, out_specs=P(("grp", "ep", "tp"), None), check_vma=False
    )
```

```python
import functools

import jax
import jax.numpy as jnp
from jax import lax
from jax.experimental import pallas as pl
from jax.experimental.pallas import tpu as pltpu
from jax.sharding import PartitionSpec as P

norm_eps = 1e-05
clamp_limit = 7.0
sig_alpha = 1.702

F32 = jnp.float32
BF16 = jnp.bfloat16
VMEM_BYTES = 67_043_328


def iota(shape, dim):
    return lax.broadcasted_iota(jnp.int32, shape, dim)


def dot(a, b):
    return jnp.dot(a, b, preferred_element_type=F32)


def routed_kernel(
    cap,
    ids_ref, gates_ref, gain_ref, tokens_hbm, wg_hbm, wu_hbm, wd_hbm,
    out_ref,
    tokens, wgu, wd, unsort, total,
    ag0, ag1, rs0, rs1, md0, md1, st0, st1,
    xin, xout, yy, yout,
    w_sem, ag_rv0, ag_rv1, rs_rv0, rs_rv1, md_rv0, md_rv1, x_rv, y_rv,
    ag_tx, rs_tx, md_tx, x_tx, y_tx,
):
    n = lax.axis_size("ep")
    cores = lax.axis_size("tp")
    me = lax.axis_index("ep")
    core = lax.axis_index("tp")
    rows, width = tokens_hbm.shape
    top = ids_ref.shape[0]
    hidden_width = wg_hbm.shape[2]
    experts = n * cores
    quad = cores * cap
    parts = rows // quad
    reach = (n // 2, n - 1 - n // 2)
    both = (0, 1)
    batch = 2 * quad
    ag, rs, md, st = (ag0, ag1), (rs0, rs1), (md0, md1), (st0, st1)
    ag_rv, rs_rv, md_rv = (ag_rv0, ag_rv1), (rs_rv0, rs_rv1), (md_rv0, md_rv1)

    turn = 1 - 2 * core
    nxt = (lax.rem(me + turn + n, n), lax.rem(me - turn + n, n))
    partner = {"tp": 1 - core}

    def copy_to(src, dst, tx, rv, device):
        return pltpu.make_async_remote_copy(
            src_ref=src, dst_ref=dst, send_sem=tx, recv_sem=rv,
            device_id=device, device_id_type=pl.DeviceIdType.MESH,
        )

    token_load = pltpu.make_async_copy(tokens_hbm, tokens, w_sem.at[3])
    token_load.start()
    loads = (
        pltpu.make_async_copy(wg_hbm.at[0], wgu.at[:, pl.ds(0, hidden_width)], w_sem.at[0]),
        pltpu.make_async_copy(wu_hbm.at[0], wgu.at[:, pl.ds(hidden_width, hidden_width)], w_sem.at[1]),
        pltpu.make_async_copy(wd_hbm.at[0], wd, w_sem.at[2]),
    )
    for load in loads:
        load.start()

    barrier = pltpu.get_barrier_semaphore()
    for device in ({"ep": nxt[0]}, {"ep": nxt[1]}, partner):
        pl.semaphore_signal(barrier, inc=1, device_id=device, device_id_type=pl.DeviceIdType.MESH)

    ids = ids_ref[...]
    lane = iota((1, rows), 1)
    hits = [ids[k:k + 1] == iota((experts, rows), 0) for k in range(top)]
    named = functools.reduce(jnp.add, [h.astype(F32) for h in hits])
    earlier = (iota((rows, rows), 0) < iota((rows, rows), 1)).astype(BF16)
    before = dot(named.astype(BF16), earlier)
    slots = [jnp.sum(jnp.where(h, before, 0.0), 0, keepdims=True) for h in hits]
    codes = [(cap * ids[k:k + 1]).astype(F32) + slots[k] for k in range(top)]
    meta = jnp.concatenate(codes + [gates_ref[k:k + 1] for k in range(top)], 0)
    meta_hi = meta.astype(BF16)
    rest = meta - meta_hi.astype(F32)
    meta_mid = rest.astype(BF16)
    meta_lo = (rest - meta_mid.astype(F32)).astype(BF16)

    away = lax.rem((ids // cores - me) * turn + 2 * n, n)
    eye = iota((rows, rows), 0) == iota((rows, rows), 1)
    place = []
    for d in range(2):
        far = away if d == 0 else n - away
        inside = (away <= reach[0]) if d == 0 else (away > reach[0])
        far = jnp.max(jnp.where(inside, far, 0), 0, keepdims=True)
        key = (far * rows + (rows - 1 - lane)).astype(F32)
        key_col = jnp.sum(jnp.where(eye, key, 0.0), 1, keepdims=True)
        rank = jnp.sum((key_col > key).astype(F32), 0, keepdims=True)
        rank_col = jnp.sum((key > key_col).astype(F32), 1, keepdims=True)
        place.append((iota((rows, rows), 0).astype(F32) == rank).astype(BF16))
        back = (iota((rows, rows), 1).astype(F32) == rank_col).astype(BF16)
        unsort[d] = back
        md[d][0:8, :] = dot(meta_hi, back) + dot(meta_mid, back) + dot(meta_lo, back)

    def sort_part(d, i):
        at = slice(quad * i, quad * (i + 1))
        values = dot(place[d][at], tokens[...])
        centred = values - jnp.mean(values, -1, keepdims=True)
        var = jnp.mean(centred * centred, -1, keepdims=True)
        ag[d][at, :] = (centred * lax.rsqrt(var + norm_eps) * gain_ref[...]).astype(BF16)

    def blank_rows():
        for d in range(2):
            for short in range(1, parts):
                h = reach[d] - parts + 1 + short
                top_row = rows * h + quad * (parts - short)
                ag[d][top_row:rows * (h + 1), :] = jnp.zeros((quad * short, width), BF16)

    def send_part(d, i, h):
        at = pl.multiple_of(rows * (h - 1) + quad * i, quad)
        if i == 0:
            m = pl.multiple_of(8 * (h - 1), 8)
            copy_to(md[d].at[pl.ds(m, 8)], md[d].at[pl.ds(m + 8, 8)],
                    md_tx.at[d], md_rv[d].at[h], {"ep": nxt[d]}).start()
        copy_to(ag[d].at[pl.ds(at, quad)], ag[d].at[pl.ds(at + rows, quad)],
                ag_tx.at[d], ag_rv[d].at[h, i], {"ep": nxt[d]}).start()

    def take_part(d, i, h):
        at = pl.multiple_of(rows * h + quad * i, quad)
        if i == 0:
            m = md[d].at[pl.ds(pl.multiple_of(8 * h, 8), 8)]
            copy_to(m, m, md_tx.at[d], md_rv[d].at[h], {"ep": nxt[d]}).wait_recv()
        part = ag[d].at[pl.ds(at, quad)]
        copy_to(part, part, ag_tx.at[d], ag_rv[d].at[h, i], {"ep": nxt[d]}).wait_recv()

    def select_block(d, b):
        j = b - d
        meta = md[d][pl.ds(pl.multiple_of(8 * j, 8), 8), :]
        row = iota((quad, rows), 0)
        want = (quad * me + lax.rem(cap * core + row, quad)).astype(F32)
        pick = jnp.zeros((quad, rows), F32)
        weight = jnp.zeros((quad, rows), F32)
        for k in range(top):
            hit = meta[k:k + 1] == want
            pick = jnp.where(hit, 1.0, pick)
            weight = jnp.where(hit, meta[top + k:top + k + 1], weight)
        block = ag[d][pl.ds(pl.multiple_of(rows * j, rows), rows), :]
        found = dot(pick.astype(BF16), block).astype(BF16)
        xin[pl.ds(pl.multiple_of(batch * (b - 1) + cap * d, cap), cap), :] = found[:cap]
        xout[pl.ds(pl.multiple_of(quad * (b - 1) + cap * d, cap), cap), :] = found[cap:]
        none = jnp.zeros((cap, rows), F32)
        mine, other = weight[:cap], weight[cap:]
        spread = (mine, none, other, none) if d == 0 else (none, mine, none, other)
        spread = jnp.concatenate(spread + (jnp.zeros((rows - batch, rows), F32),), 0)
        st[d][pl.ds(pl.multiple_of(rows * j, rows), rows), :] = spread.T.astype(BF16)

    def select_batch(b):
        for d in both:
            select_block(d, b)
        x_copy(b).start()

    def x_copy(b):
        return copy_to(xout.at[pl.ds(pl.multiple_of(quad * (b - 1), quad), quad)],
                       xin.at[pl.ds(pl.multiple_of(batch * (b - 1) + quad, quad), quad)],
                       x_tx, x_rv.at[b - 1], partner)

    def y_copy(b):
        return copy_to(yout.at[pl.ds(pl.multiple_of(quad * (b - 1), quad), quad)],
                       yy.at[pl.ds(pl.multiple_of(batch * (b - 1) + quad, quad), quad)],
                       y_tx, y_rv.at[b - 1], partner)

    def expert_batch(b):
        x_copy(b).wait_recv()
        at = pl.multiple_of(batch * (b - 1), batch)
        pre = dot(xin[pl.ds(at, batch), :], wgu[...])
        gated = jnp.minimum(pre[:, :hidden_width], clamp_limit)
        upper = jnp.clip(pre[:, hidden_width:], -clamp_limit, clamp_limit)
        hidden = (gated * jax.nn.sigmoid(sig_alpha * gated) * (upper + 1.0)).astype(BF16)
        result = dot(hidden, wd[...]).astype(BF16)
        yy[pl.ds(at, quad), :] = result[:quad]
        yout[pl.ds(pl.multiple_of(quad * (b - 1), quad), quad), :] = result[quad:]
        y_copy(b).start()

    def y_wait(b):
        y_copy(b).wait_recv()

    def share_of(d, j, at, count):
        results = yy[pl.ds(pl.multiple_of(batch * (j + d - 1), batch), batch), :]
        return dot(st[d][pl.ds(at, count), :][:, :batch], results)

    def give_part(d, j, i, fresh=False):
        at = pl.multiple_of(rows * j + quad * i, quad)
        share = share_of(d, j, at, quad)
        part = rs[d].at[pl.ds(at, quad)]
        if not fresh:
            copy_to(part, part, rs_tx.at[d], rs_rv[d].at[j, i], {"ep": nxt[d]}).wait_recv()
            share = share + part[...].astype(F32)
        part[...] = share.astype(BF16)
        copy_to(part, rs[d].at[pl.ds(at - rows, quad)], rs_tx.at[d], rs_rv[d].at[j - 1, i],
                {"ep": nxt[1 - d]}).start()

    def pass_on(d, i, h):
        take_part(d, i, h)
        send_part(d, i, h + 1)

    token_load.wait()
    sort_part(0, 0)
    pl.semaphore_wait(barrier, 3)
    send_part(0, 0, 1)
    sort_part(0, 1)
    send_part(0, 1, 1)
    sort_part(0, 2)
    send_part(0, 2, 1)
    pass_on(0, 0, 1)
    sort_part(1, 0)
    send_part(1, 0, 1)
    pass_on(0, 1, 1)
    sort_part(1, 1)
    send_part(1, 1, 1)
    pass_on(0, 0, 2)
    sort_part(1, 2)
    send_part(1, 2, 1)
    sort_part(0, 3)
    send_part(0, 3, 1)
    pass_on(1, 0, 1)
    pass_on(0, 0, 3)
    pass_on(1, 1, 1)
    pass_on(0, 1, 2)
    pass_on(1, 0, 2)
    pass_on(0, 2, 1)
    sort_part(1, 3)
    blank_rows()
    for load in loads:
        load.wait()

    last = reach[0] - parts + 1

    def round_body(r, carry):
        pass_on(0, 3, r - 1)

        @pl.when(r > 2)
        def _():
            take_part(1, 3, r - 2)

        send_part(1, 3, r - 1)
        select_batch(r - 1)
        for i in range(3):
            pass_on(0, i, r + 2 - i)
            pass_on(1, i, r + 1 - i)
            if i == 1:
                expert_batch(r - 1)
        return carry

    lax.fori_loop(2, last + 1, round_body, 0)

    def y_wait_body(b, carry):
        y_wait(b)
        return carry

    order = (parts - 1,) + tuple(range(parts - 1))
    lax.fori_loop(1, last, y_wait_body, 0)
    for step in range(parts + 1):
        if step < parts:
            for d in both:
                take_part(d, order[step], reach[d] - order[step])
            select_batch(reach[0] - order[step])
        if step > 0:
            expert_batch(reach[0] - order[step - 1])
            if step > 1:
                y_wait(reach[0] - order[step - 2])
                for d in both:
                    give_part(d, reach[d] - order[step - 2], order[step - 2], True)
    y_wait(reach[0] - order[-1])
    for d in both:
        give_part(d, reach[d] - order[-1], order[-1], True)

    for i in order:
        give_part(0, reach[0] - i - 1, i)

    def give_body(r, carry):
        for i in order:
            for d in both:
                give_part(d, reach[0] - i - r, i)
        return carry

    lax.fori_loop(2, last, give_body, 0)
    for j, i in ((3, 0), (2, 1), (1, 2), (2, 0), (1, 1), (1, 0)):
        for d in both:
            give_part(d, j, i)

    def home_part(d, i):
        part = rs[d].at[pl.ds(quad * i, quad)]
        copy_to(part, part, rs_tx.at[d], rs_rv[d].at[0, i], {"ep": nxt[d]}).wait_recv()

    half = rows // 2
    own = dot(unsort[1], st1[0:rows, :]).astype(BF16)[:, :batch]
    for d in both:
        for i in range(parts // 2, parts):
            home_part(d, i)
    total[...] = (
        dot(own, yy[0:batch, :])
        + dot(unsort[0][:, half:], rs0[half:rows, :])
        + dot(unsort[1][:, half:], rs1[half:rows, :])
    )
    for i in reversed(range(parts // 2)):
        for d in both:
            home_part(d, i)
    out_ref[...] = (
        total[...] + dot(unsort[0][:, :half], rs0[0:half, :]) + dot(unsort[1][:, :half], rs1[0:half, :])
    ).astype(BF16)

    for d in both:
        moved = quad * sum(reach[d] - i for i in range(parts))
        sent = ag[d].at[pl.ds(0, moved)]
        copy_to(sent, sent, ag_tx.at[d], ag_rv[d].at[0, 0], {"ep": nxt[d]}).wait_send()
        sent = rs[d].at[pl.ds(0, moved)]
        copy_to(sent, sent, rs_tx.at[d], rs_rv[d].at[0, 0], {"ep": nxt[d]}).wait_send()
        sent = md[d].at[pl.ds(0, 8 * reach[d])]
        copy_to(sent, sent, md_tx.at[d], md_rv[d].at[0], {"ep": nxt[d]}).wait_send()
    copy_to(xout, xout, x_tx, x_rv.at[0], partner).wait_send()
    copy_to(yout, yout, y_tx, y_rv.at[0], partner).wait_send()


def local(tokens, expert_ids, route_weights, norm_gain, w_gate, w_up, w_down):
    n = lax.axis_size("ep")
    cores = lax.axis_size("tp")
    rows, width = tokens.shape
    top = expert_ids.shape[1]
    hidden_width = w_gate.shape[2]
    cap = 2 * rows * top // (n * cores)
    quad = cores * cap
    parts = rows // quad
    reach = (n // 2, n - 1 - n // 2)
    batches = reach[0]
    vmem = pl.BlockSpec(memory_space=pltpu.VMEM)
    hbm = pl.BlockSpec(memory_space=pl.ANY)
    dma = pltpu.SemaphoreType.DMA
    blocks = [pltpu.VMEM((rows * (r + 1), width), BF16) for r in reach]
    return pl.pallas_call(
        functools.partial(routed_kernel, cap),
        name="routed_layer",
        out_shape=jax.ShapeDtypeStruct((rows, width), BF16),
        in_specs=[vmem] * 3 + [hbm] * 4,
        out_specs=vmem,
        scratch_shapes=[
            pltpu.VMEM((rows, width), BF16),
            pltpu.VMEM((width, 2 * hidden_width), BF16),
            pltpu.VMEM((hidden_width, width), BF16),
            pltpu.VMEM((2, rows, rows), BF16),
            pltpu.VMEM((rows, width), F32),
            *blocks,
            *blocks,
            *[pltpu.VMEM((8 * (r + 1), rows), F32) for r in reach],
            *[pltpu.VMEM((rows * (r + 1), rows), BF16) for r in reach],
            pltpu.VMEM((2 * quad * batches, width), BF16),
            pltpu.VMEM((quad * batches, width), BF16),
            pltpu.VMEM((2 * quad * batches, width), BF16),
            pltpu.VMEM((quad * batches, width), BF16),
            dma((4,)),
            *[dma((r + 1, parts)) for r in reach],
            *[dma((r + 1, parts)) for r in reach],
            *[dma((r + 1,)) for r in reach],
            dma((batches,)),
            dma((batches,)),
            dma((2,)),
            dma((2,)),
            dma((2,)),
            dma,
            dma,
        ],
        compiler_params=pltpu.CompilerParams(
            collective_id=0, has_side_effects=True, vmem_limit_bytes=VMEM_BYTES
        ),
    )(expert_ids.T, route_weights.T, norm_gain.reshape(1, width), tokens, w_gate, w_up, w_down)


def solution(mesh):
    placed = (
        P(("grp", "ep", "tp"), None),
        P(("grp", "ep", "tp"), None),
        P(("grp", "ep", "tp"), None),
        P(),
        P(("ep", "tp"), None, None),
        P(("ep", "tp"), None, None),
        P(("ep", "tp"), None, None),
    )
    return jax.shard_map(
        local, mesh=mesh, in_specs=placed, out_specs=P(("grp", "ep", "tp"), None), check_vma=False
    )
```
